32 devices in a mesh: grp: 2 (over y), fs: 4 (over z), tp: 4 (over x, core).
Axes of the slice: x: 2, y: 2, z: 4, core: 2. Of those that a mesh axis runs over, the one named last changes fastest.
Arguments:
- hidden_activations: bfloat16 [2048, 6144], P('tp', ('grp', 'fs')), parts along dimension 1, may hold values from -6 to 6
- attention_rescaling_factors: float32 [2048], replicated, may hold values from 0.1 to 1.9
- feature_rescaling_factors: float32 [2048], replicated, may hold values from 0.1 to 1.9
- request_matrix: float32 [2048, 2048], P('fs', 'tp'), may hold values from -0.125 to 0.125
- request_matrix_multipliers: float32 [2048], P('tp'), may hold values from 0.1 to 1.9
- lookup_matrix: float32 [2048, 2048], P('fs', 'tp'), may hold values from -0.125 to 0.125
- lookup_matrix_multipliers: float32 [2048], P('tp'), may hold values from 0.1 to 1.9
- content_matrix: float32 [2048, 4096], P('fs', 'tp'), may hold values from -0.125 to 0.125
- content_matrix_multipliers: float32 [4096], P('tp'), may hold values from 0.1 to 1.9
- valve_matrix: float32 [2048, 4096], P('fs', 'tp'), may hold values from -0.125 to 0.125
- valve_matrix_multipliers: float32 [4096], P('tp'), may hold values from 0.1 to 1.9
- result_matrix: float32 [4096, 2048], P('tp', 'fs'), may hold values from -0.09375 to 0.09375
- result_matrix_multipliers: float32 [2048], P('fs'), may hold values from 0.1 to 1.9
- expanding_matrix: float32 [2048, 8192], P('fs', 'tp'), may hold values from -0.125 to 0.125
- expand_matrix_multipliers: float32 [8192], P('tp'), may hold values from 0.1 to 1.9
- shrinking_matrix: float32 [8192, 2048], P('tp', 'fs'), may hold values from -0.0625 to 0.0625
- shrink_matrix_multipliers: float32 [2048], P('fs'), may hold values from 0.1 to 1.9
- attention_fading_logarithm: float32 [8], P('tp'), may hold values from -1 to 0
- spike_fading_logarithm: float32 [8, 6144], P('tp', ('grp', 'fs')), parts along dimension 1, may hold values from -1 to 0, as said below
Outputs:
- out_stream: bfloat16 [2048, 6144], P('tp', ('grp', 'fs')), parts along dimension 1
The draws below stay inside these ranges and needn't reach their ends.
There are 2 independent parts, one for each index of `grp`. The reference program is written for one: setup_inputs(seed, part) draws one part's arguments, and reference() takes and returns one part's arrays. A program takes and returns all parts, laid end to end along the dimension named above; an argument that names none is the same for every part. Nothing has to cross between parts.
Inputs may be any that keep to these rules, and one draw needn't show every extreme that they name: `spike_fading_logarithm`: log decay added to the head's own.
All inputs are finite; a program needn't handle non-finite values.
Results may differ from the reference program's by a relative error of at most 0.019.
Values may be sent and summed in bfloat16 or wider, within the bound.
A program may use at most 128 MiB of HBM per device.

```python
import jax
import jax.numpy as jnp
from jax import lax

D = 2048
DK = 256
DV = 512
HEADS = 8
FF = 8192
BLOCK_POSITIONS = 128
LEN = 768
TOKENS = 3072


def draw_attention_fading_logarithm(key, part):
    flag_key, fast_key, slow_key = jax.random.split(key, 3)
    fast_share = 0.5
    fast_flags = jax.random.bernoulli(flag_key, fast_share, (HEADS,))
    fast_rate = -3.0 / jax.random.uniform(fast_key, (HEADS,), jnp.float32, 30.0, 100.0)
    slow_rate = -jax.random.uniform(slow_key, (HEADS,), jnp.float32, 0.1, 0.8) / LEN
    return jnp.where(fast_flags, fast_rate, slow_rate).astype(jnp.float32)


def draw_spike_fading_logarithm(key, part):
    place_key, depth_key = jax.random.split(key)
    places = jax.random.bernoulli(place_key, 2.0 / LEN, (1, TOKENS))
    depths = jnp.log(jax.random.uniform(depth_key, (HEADS, TOKENS), jnp.float32, 0.5, 0.8))
    return jnp.where(places, depths, 0.0).astype(jnp.float32)


def block_scale(rng, dims, shards, least, top_value):
    def one(axis_at, blocks):
        draws = jax.random.uniform(jax.random.fold_in(jax.random.fold_in(rng, 6), axis_at), (blocks,), jnp.float32, least / len(shards), top_value / len(shards))
        return jnp.repeat(jnp.exp(draws), dims[axis_at] // blocks).reshape((-1,) + (1,) * (len(dims) - axis_at - 1))

    level = one(*shards[0])
    for cut in shards[1:]:
        level = level * one(*cut)
    return level


def normal_values(stream_key, dims, deviation, limit, pieces=(), held_as=jnp.bfloat16):
    drawn = jax.random.normal(stream_key, dims, jnp.float32) * deviation
    if len(pieces) > 0:
        drawn = block_scale(stream_key, dims, pieces, -0.22, 0.18) * drawn
    return jnp.clip(drawn, min=-limit, max=limit).astype(held_as)


def setup_inputs(seed: int = 0, part: int = 0) -> dict:
    key_list = jax.random.split(jax.random.key(seed), 20)
    own_keys = jax.random.split(jax.random.fold_in(key_list[19], part), 20)
    return {
        "hidden_activations": normal_values(own_keys[0], (D, TOKENS), 1.0, 6.0, ((0, 4), (1, 4))),
        "attention_rescaling_factors": jnp.clip(1.0 + 0.18 * jax.random.normal(key_list[1], (D,), jnp.float32), 0.1, 1.9),
        "feature_rescaling_factors": jnp.clip(1.0 + 0.18 * jax.random.normal(key_list[2], (D,), jnp.float32), 0.1, 1.9),
        "request_matrix": normal_values(key_list[3], (D, D), D ** -0.5, 0.125, ((0, 4), (1, 4)), jnp.float32),
        "request_matrix_multipliers": jnp.clip(1.0 + 0.18 * jax.random.normal(key_list[4], (D,), jnp.float32), 0.1, 1.9),
        "lookup_matrix": normal_values(key_list[5], (D, D), D ** -0.5, 0.125, ((0, 4), (1, 4)), jnp.float32),
        "lookup_matrix_multipliers": jnp.clip(1.0 + 0.18 * jax.random.normal(key_list[6], (D,), jnp.float32), 0.1, 1.9),
        "content_matrix": normal_values(key_list[7], (D, 2 * D), D ** -0.5, 0.125, ((0, 4), (1, 4)), jnp.float32),
        "content_matrix_multipliers": jnp.clip(1.0 + 0.18 * jax.random.normal(key_list[8], (2 * D,), jnp.float32), 0.1, 1.9),
        "valve_matrix": normal_values(key_list[9], (D, 2 * D), D ** -0.5, 0.125, ((0, 4), (1, 4)), jnp.float32),
        "valve_matrix_multipliers": jnp.clip(1.0 + 0.18 * jax.random.normal(key_list[10], (2 * D,), jnp.float32), 0.1, 1.9),
        "result_matrix": normal_values(key_list[11], (2 * D, D), (2 * D) ** -0.5, 0.09375, ((0, 4), (1, 4)), jnp.float32),
        "result_matrix_multipliers": jnp.clip(1.0 + 0.18 * jax.random.normal(key_list[12], (D,), jnp.float32), 0.1, 1.9),
        "expanding_matrix": normal_values(key_list[13], (D, FF), D ** -0.5, 0.125, ((0, 4), (1, 4)), jnp.float32),
        "expand_matrix_multipliers": jnp.clip(1.0 + 0.18 * jax.random.normal(key_list[14], (FF,), jnp.float32), 0.1, 1.9),
        "shrinking_matrix": normal_values(key_list[15], (FF, D), FF ** -0.5, 0.0625, ((0, 4), (1, 4)), jnp.float32),
        "shrink_matrix_multipliers": jnp.clip(1.0 + 0.18 * jax.random.normal(key_list[16], (D,), jnp.float32), 0.1, 1.9),
        "attention_fading_logarithm": draw_attention_fading_logarithm(jax.random.fold_in(key_list[19], 71), part),
        "spike_fading_logarithm": draw_spike_fading_logarithm(jax.random.fold_in(jax.random.fold_in(key_list[19], part), 71), part),
    }


epsilon = 1e-06

def rms_norm(matrix, norm_gain):
    values = matrix.astype(jnp.float32)
    factor = lax.rsqrt(lax.optimization_barrier(jnp.mean(values * values, axis=0, keepdims=True)) + epsilon)
    return (values * factor * norm_gain[:, None]).astype(jnp.bfloat16)

def project(normed, weight):
    return lax.dot_general(normed, weight.astype(jnp.bfloat16), (((0,), (0,)), ((), ())), preferred_element_type=jnp.float32)

def widen(array):
    return lax.optimization_barrier(array).astype(jnp.float32)

def retain(query, keys, values, fading_logarithm_speed):
    length = query.shape[2]
    causal = jnp.arange(length)[:, None] >= jnp.arange(length)[None, :]

    def advance(memory, inputs):
        query_blk, key_blk, value_blk, rate_blk = inputs
        running = jnp.cumsum(rate_blk, axis=-1)
        closing = running[:, -1:]
        spread = jnp.where(causal, running[:, :, None] - running[:, None, :], 0.0)
        decays = jnp.where(causal, jnp.exp(spread), 0.0)
        query_wide = query_blk.astype(jnp.float32)
        value_wide = value_blk.astype(jnp.float32)
        scores = jnp.einsum('gid,gjd->gij', query_wide, key_blk.astype(jnp.float32)) * decays
        weights = widen(scores.astype(jnp.bfloat16))
        within = jnp.einsum('gij,gjv->giv', weights, value_wide)
        state_copy = widen(memory.astype(jnp.bfloat16))
        carried = jnp.einsum('gid,gdv->giv', query_wide, state_copy) * jnp.exp(running)[:, :, None]
        faded_keys = widen((key_blk.astype(jnp.float32) * jnp.exp(closing - running)[:, :, None]).astype(jnp.bfloat16))
        memory = memory * jnp.exp(closing)[:, :, None] + jnp.einsum('gjd,gjv->gdv', faded_keys, value_wide)
        return (memory, within + carried)
    initial = jnp.zeros((query.shape[0], query.shape[3], values.shape[3]), jnp.float32)
    stacked = tuple((jnp.swapaxes(member, 0, 1) for member in (query, keys, values, fading_logarithm_speed)))
    _, outputs = lax.scan(advance, initial, stacked)
    return jnp.swapaxes(outputs, 0, 1)

def group_norm(retained):
    center = lax.optimization_barrier(jnp.mean(retained, axis=-1, keepdims=True))
    offset = retained - center
    variance = lax.optimization_barrier(jnp.mean(offset * offset, axis=-1, keepdims=True))
    return offset * lax.rsqrt(variance + epsilon)

def reference(hidden_activations, attention_rescaling_factors, feature_rescaling_factors, request_matrix, request_matrix_multipliers, lookup_matrix, lookup_matrix_multipliers, content_matrix, content_matrix_multipliers, valve_matrix, valve_matrix_multipliers, result_matrix, result_matrix_multipliers, expanding_matrix, expand_matrix_multipliers, shrinking_matrix, shrink_matrix_multipliers, attention_fading_logarithm, spike_fading_logarithm):
    sequences = TOKENS // LEN
    blocks = LEN // BLOCK_POSITIONS
    normed = rms_norm(hidden_activations, attention_rescaling_factors)
    query = (project(normed, request_matrix) * request_matrix_multipliers).astype(jnp.bfloat16)
    keys = (project(normed, lookup_matrix) * lookup_matrix_multipliers * DK ** (-0.5)).astype(jnp.bfloat16)
    values = (project(normed, content_matrix) * content_matrix_multipliers).astype(jnp.bfloat16)
    gate = project(normed, valve_matrix) * valve_matrix_multipliers

    def to_heads(matrix, width):
        split = matrix.reshape(sequences, blocks, BLOCK_POSITIONS, HEADS, width)
        return jnp.transpose(split, (0, 3, 1, 2, 4)).reshape(sequences * HEADS, blocks, BLOCK_POSITIONS, width)
    fading_logarithm_speed = attention_fading_logarithm[:, None] + spike_fading_logarithm
    rate_blocks = jnp.transpose(fading_logarithm_speed.reshape(HEADS, sequences, blocks, BLOCK_POSITIONS), (1, 0, 2, 3)).reshape(sequences * HEADS, blocks, BLOCK_POSITIONS)
    retained = retain(to_heads(query, DK), to_heads(keys, DK), to_heads(values, DV), rate_blocks)
    retained = jnp.transpose(retained.reshape(sequences, HEADS, blocks, BLOCK_POSITIONS, DV), (0, 2, 3, 1, 4)).reshape(TOKENS, HEADS, DV)
    heads_out = (group_norm(retained).reshape(TOKENS, HEADS * DV) * jax.nn.silu(gate)).astype(jnp.bfloat16)
    update = lax.dot_general(result_matrix.astype(jnp.bfloat16), heads_out, (((0,), (1,)), ((), ())), preferred_element_type=jnp.float32) * result_matrix_multipliers[:, None]
    middle = (hidden_activations.astype(jnp.float32) + update).astype(jnp.bfloat16)
    normed_mlp = rms_norm(middle, feature_rescaling_factors)
    rising = jax.nn.relu(project(normed_mlp, expanding_matrix) * expand_matrix_multipliers)
    hidden = (rising * rising).astype(jnp.bfloat16)
    lowered = lax.dot_general(shrinking_matrix.astype(jnp.bfloat16), hidden, (((0,), (1,)), ((), ())), preferred_element_type=jnp.float32) * shrink_matrix_multipliers[:, None]
    return (middle.astype(jnp.float32) + lowered).astype(jnp.bfloat16)
```

```python
import jax
import jax.numpy as jnp
from jax import lax
from jax.sharding import PartitionSpec as P


DK = 256
DV = 512


epsilon = 1e-06


def rms_norm(matrix, norm_gain):
    values = matrix.astype(jnp.float32)
    factor = lax.rsqrt(jnp.mean(values * values, axis=0, keepdims=True) + epsilon)
    return (values * factor * norm_gain[:, None]).astype(jnp.bfloat16)


def project(normed, weight):
    return lax.dot_general(
        normed, weight, (((0,), (0,)), ((), ())), preferred_element_type=jnp.float32
    )


def collect_features(matrix):
    return lax.all_gather(matrix, "tp", axis=0, tiled=True)


def group_norm(retained):
    center = jnp.mean(retained, axis=-1, keepdims=True)
    offset = retained - center
    variance = jnp.mean(offset * offset, axis=-1, keepdims=True)
    return offset * lax.rsqrt(variance + epsilon)


def retain(query, keys, values, rates):
    length, heads = query.shape[0], rates.shape[0]
    causal = jnp.arange(length)[:, None] >= jnp.arange(length)[None, :]
    running = jnp.cumsum(rates, axis=-1)
    outputs = []
    for head in range(heads):
        head_query = query[:, head * DK : (head + 1) * DK]
        head_keys = keys[:, head * DK : (head + 1) * DK]
        head_values = values[:, head * DV : (head + 1) * DV]
        spread = jnp.where(causal, running[head, :, None] - running[head, None, :], 0.0)
        decays = jnp.where(causal, jnp.exp(spread), 0.0)
        scores = lax.dot_general(
            head_query, head_keys, (((1,), (1,)), ((), ())), preferred_element_type=jnp.float32
        )
        weights = (scores * decays).astype(jnp.bfloat16)
        outputs.append(
            lax.dot_general(
                weights, head_values, (((1,), (0,)), ((), ())), preferred_element_type=jnp.float32
            )
        )
    return outputs


def make_local(ring_size, copies):
    ring = [(at, (at + 1) % ring_size) for at in range(ring_size)]

    def ring_step(block):
        return lax.ppermute(block, "fs", ring)

    def swap(block, shift):
        return lax.ppermute(
            block, "grp", [(at, (at - shift) % copies) for at in range(copies)]
        )

    def local(
        hidden_activations,
        attention_rescaling_factors,
        feature_rescaling_factors,
        request_matrix,
        request_matrix_multipliers,
        lookup_matrix,
        lookup_matrix_multipliers,
        content_matrix,
        content_matrix_multipliers,
        valve_matrix,
        valve_matrix_multipliers,
        result_matrix,
        result_matrix_multipliers,
        expanding_matrix,
        expand_matrix_multipliers,
        shrinking_matrix,
        shrink_matrix_multipliers,
        attention_fading_logarithm,
        spike_fading_logarithm,
    ):
        fs, grp = lax.axis_index("fs"), lax.axis_index("grp")
        bf16 = jnp.bfloat16

        def owner(hop):
            return (fs - hop) % ring_size

        def part(shift):
            return (grp + shift) % copies

        def chain(shard, axis):
            size = shard.shape[axis] // copies
            pieces = [
                [
                    lax.dynamic_slice_in_dim(shard, part(shift) * size, size, axis).astype(bf16)
                    for shift in range(copies)
                ]
            ]
            block = pieces[0][0]
            for _ in range(1, ring_size):
                block = ring_step(block)
                pieces.append([block] + [swap(block, shift) for shift in range(1, copies)])
            return pieces

        def rows_of(matrix):
            size = matrix.shape[0] // (ring_size * copies)
            return jnp.concatenate(
                [
                    lax.dynamic_slice_in_dim(
                        matrix, (owner(hop) * copies + part(shift)) * size, size, 0
                    )
                    for hop in range(ring_size)
                    for shift in range(copies)
                ],
                axis=0,
            )

        def stack(pieces):
            return jnp.concatenate([piece for hop in pieces for piece in hop], axis=0)

        def columns(pieces):
            rows, size = pieces[0][0].shape
            whole = jnp.zeros((rows, size * ring_size * copies), bf16)
            for hop in range(ring_size):
                for shift in range(copies):
                    start = (owner(hop) * copies + part(shift)) * size
                    whole = lax.dynamic_update_slice(whole, pieces[hop][shift], (0, start))
            return whole

        scales = jnp.stack([result_matrix_multipliers, shrink_matrix_multipliers])
        every_scale = jnp.zeros((2, scales.shape[1] * ring_size), jnp.float32)
        block = scales
        for hop in range(ring_size):
            if hop:
                block = ring_step(block)
            every_scale = lax.dynamic_update_slice(
                every_scale, block, (0, owner(hop) * scales.shape[1])
            )
        out_scales, down_scales = every_scale[0], every_scale[1]

        half_up = expanding_matrix.shape[1] // 2
        half_down = shrinking_matrix.shape[0] // 2
        qk = chain(jnp.concatenate([request_matrix, lookup_matrix], axis=1), 0)
        v = chain(content_matrix, 0)
        gates = chain(valve_matrix, 0)
        out = chain(result_matrix, 1)
        ups = [chain(expanding_matrix[:, :half_up], 0), chain(expanding_matrix[:, half_up:], 0)]
        downs = [chain(shrinking_matrix[:half_down], 1), chain(shrinking_matrix[half_down:], 1)]

        normed = rows_of(
            rms_norm(collect_features(hidden_activations), attention_rescaling_factors)
        )
        width = request_matrix.shape[1]
        qk_sum = project(normed, stack(qk))
        query = (qk_sum[:, :width] * request_matrix_multipliers).astype(bf16)
        keys = (qk_sum[:, width:] * lookup_matrix_multipliers * DK ** (-0.5)).astype(bf16)
        values = (project(normed, stack(v)) * content_matrix_multipliers).astype(bf16)
        rates = attention_fading_logarithm[:, None] + spike_fading_logarithm
        retained = retain(query, keys, values, rates)
        gate = project(normed, stack(gates)) * valve_matrix_multipliers
        heads_out = jnp.concatenate(
            [
                (
                    group_norm(retained[head])
                    * jax.nn.silu(gate[:, head * DV : (head + 1) * DV])
                ).astype(bf16)
                for head in range(len(retained))
            ],
            axis=1,
        )
        update = lax.psum_scatter(
            (
                lax.dot_general(
                    columns(out),
                    heads_out,
                    (((0,), (1,)), ((), ())),
                    preferred_element_type=jnp.float32,
                )
                * out_scales[:, None]
            ).astype(bf16),
            "tp",
            scatter_dimension=0,
            tiled=True,
        ).astype(jnp.float32)
        middle = (hidden_activations.astype(jnp.float32) + update).astype(bf16)
        normed_mlp = rows_of(rms_norm(collect_features(middle), feature_rescaling_factors))
        terms = None
        for side in range(2):
            scale = expand_matrix_multipliers[side * half_up : (side + 1) * half_up]
            rising = jax.nn.relu(project(normed_mlp, stack(ups[side])) * scale)
            hidden = (rising * rising).astype(bf16)
            term = lax.dot_general(
                columns(downs[side]),
                hidden,
                (((0,), (1,)), ((), ())),
                preferred_element_type=jnp.float32,
            )
            terms = term if terms is None else terms + term
        lowered = lax.psum_scatter(
            (terms * down_scales[:, None]).astype(bf16), "tp", scatter_dimension=0, tiled=True
        ).astype(jnp.float32)
        return (middle.astype(jnp.float32) + lowered).astype(bf16)

    return local


def solution(mesh):
    ring_size, copies = mesh.shape["fs"], mesh.shape["grp"]
    placed = (
        P("tp", ("grp", "fs")),
        P(),
        P(),
        P("fs", "tp"),
        P("tp"),
        P("fs", "tp"),
        P("tp"),
        P("fs", "tp"),
        P("tp"),
        P("fs", "tp"),
        P("tp"),
        P("tp", "fs"),
        P("fs"),
        P("fs", "tp"),
        P("tp"),
        P("tp", "fs"),
        P("fs"),
        P("tp"),
        P("tp", ("grp", "fs")),
    )
    return jax.shard_map(
        make_local(ring_size, copies),
        mesh=mesh,
        in_specs=placed,
        out_specs=P("tp", ("grp", "fs")),
        check_vma=False,
    )
```
